32 devices in a mesh: gr: 2 (over x), fs: 8 (over z, y), tp: 2 (over core).
Axes of the slice: x: 2, y: 2, z: 4, core: 2. Of those that a mesh axis runs over, the one named last changes fastest.
Arguments:
- tokens: bfloat16 [4, 2048, 2048], P(('gr', 'tp')), may hold values from -6 to 6
- gate_master: float32 [3, 2048, 7168], P(None, 'fs', ('gr', 'tp')), may hold values from -0.125 to 0.125
- up_master: float32 [3, 2048, 7168], P(None, 'fs', ('gr', 'tp')), may hold values from -0.125 to 0.125
- down_master: float32 [3, 7168, 2048], P(None, 'fs', ('gr', 'tp')), may hold values from -0.0625 to 0.0625
- norm_gain: float32 [2048], P('fs'), may hold values from 0.1 to 1.9
- route: int32 [4, 2048, 2], P(('gr', 'tp')), may hold values from 0 to 2, all different within a row
- route_weight: float32 [4, 2048, 2], P(('gr', 'tp')), may hold values from 0.05 to 1
Outputs:
- gate_out: bfloat16 [3, 2048, 7168], P(None, None, 'fs')
- up_out: bfloat16 [3, 2048, 7168], P(None, None, 'fs')
- down_out: bfloat16 [3, 7168, 2048], P(None, 'fs')
- mixed: bfloat16 [4, 2048, 2048], P(('gr', 'tp'), 'fs')
The draws below stay inside these ranges and needn't reach their ends.
Inputs may be any that keep to these rules, and one draw needn't show every extreme that they name: `route`: each token names two different experts; every expert is named by some token.
All inputs are finite; a program needn't handle non-finite values.
Results may differ from the reference program's by a relative error of at most 0.024.
Values may be sent and summed in bfloat16 or wider, within the bound.
A program may use at most 192 MiB of HBM per device.

```python
import math
import jax
import jax.numpy as jnp
from jax import lax

D = 2048
FF = 7168
EXPERTS = 3
ROWS = 2048
REQ = 4
N_FS = 8


def steps_of(rng, shape, shards, low, largest):
    level, own = 1.0, jax.random.fold_in(rng, 6)
    for position, blocks in shards:
        heights = jnp.exp(jax.random.uniform(jax.random.fold_in(own, position), (blocks,), jnp.float32, low / len(shards), largest / len(shards)))
        level = level * jnp.repeat(heights, shape[position] // blocks).reshape([-1 if axis == position else 1 for axis in range(len(shape))])
    return level


def choose_distinct(rng, rows, number_of, top, lift):
    sequence = jax.random.permutation(jax.random.fold_in(rng, 1), number_of)
    boost = sequence
    for power in range(3):
        boost = boost * boost // number_of
    boost = boost * lift // number_of
    lots = jax.random.randint(jax.random.fold_in(rng, 2), (rows, number_of), 0, 4096) + boost
    holders = jax.random.permutation(jax.random.fold_in(rng, 3), rows)[jnp.arange(number_of) % rows]
    lots = jnp.where(jnp.arange(rows)[:, None] == holders[None, :], 1 << 14, lots)
    score = lots * number_of + jnp.arange(number_of)
    return lax.top_k(score.astype(jnp.int32), top)[1].astype(jnp.int32)


def gaussian(own_key, dims, spread, bound, split=(), held_as=jnp.bfloat16):
    values = jax.random.normal(own_key, dims, jnp.float32) * spread
    if len(split) > 0:
        values = steps_of(own_key, dims, split, -0.22, 0.18) * values
    return jnp.clip(values, min=-bound, max=bound).astype(held_as)


def setup_inputs(seed: int = 0) -> dict:
    seeds = jax.random.split(jax.random.key(seed), 8)
    tokens = gaussian(seeds[0], (REQ, ROWS, D), 1.0, 6.0, ((0, 4),))
    gate_master = gaussian(seeds[1], (EXPERTS, D, FF), D ** -0.5, 0.125, ((1, 8), (2, 4)), jnp.float32)
    up_master = gaussian(seeds[2], (EXPERTS, D, FF), D ** -0.5, 0.125, ((1, 8), (2, 4)), jnp.float32)
    down_master = gaussian(seeds[3], (EXPERTS, FF, D), FF ** -0.5, 0.0625, ((1, 8), (2, 4)), jnp.float32)
    norm_gain = jnp.clip(1.0 + 0.18 * jax.random.normal(seeds[4], (D,), jnp.float32), 0.1, 1.9)
    route = choose_distinct(seeds[5], REQ * ROWS, EXPERTS, 2, 0).reshape((REQ, ROWS, 2))
    route_weight = jnp.clip(jnp.exp(math.log(1.0) - 2.9957323 * jax.random.uniform(seeds[6], (REQ, ROWS, 2), jnp.float32) ** steps_of(seeds[6], (REQ, ROWS, 2), ((0, 4),), -0.2, 0.2)), 0.05, 1.0)
    return {"tokens": tokens, "gate_master": gate_master, "up_master": up_master, "down_master": down_master, "norm_gain": norm_gain, "route": route, "route_weight": route_weight}


def normalize(rows_in):
    values = rows_in.astype(jnp.float32)
    scaled = values * lax.rsqrt(lax.optimization_barrier(jnp.mean(values * values, axis=-1, keepdims=True)) + 1e-06)
    return scaled.astype(jnp.bfloat16)

def mixing(chosen, weights):
    share = weights / lax.optimization_barrier(jnp.sum(weights, axis=-1, keepdims=True))
    labels = jnp.arange(EXPERTS, dtype=jnp.int32)
    match = (chosen[:, :, None] == labels[None, None, :]).astype(jnp.float32)
    return lax.optimization_barrier(jnp.sum(share[:, :, None] * match, axis=1))

def reference(tokens, gate_master, up_master, down_master, norm_gain, route, route_weight):
    scaled_gain = norm_gain[None, :, None]
    gate_out = (scaled_gain * gate_master).astype(jnp.bfloat16)
    up_out = (scaled_gain * up_master).astype(jnp.bfloat16)
    down_out = down_master.astype(jnp.bfloat16)
    block_width = FF // N_FS

    def one_batch(batch):
        rows_in, chosen, weights = batch
        normed = normalize(rows_in)
        combine = mixing(chosen, weights)
        hidden_list = []
        for index in range(EXPERTS):
            gate_act = jnp.dot(normed, gate_out[index], preferred_element_type=jnp.float32)
            up_act = jnp.dot(normed, up_out[index], preferred_element_type=jnp.float32)
            hidden_list.append((jax.nn.silu(gate_act) * up_act).astype(jnp.bfloat16))

        def add_block(block, total):
            start = (block * block_width).astype(jnp.int32)
            partial_sum = jnp.zeros((rows_in.shape[0], rows_in.shape[1]), jnp.float32)
            for index in range(EXPERTS):
                hidden_part = lax.dynamic_slice_in_dim(hidden_list[index], start, block_width, 1)
                down_part = lax.dynamic_slice_in_dim(down_out[index], start, block_width, 0)
                projected = jnp.dot(hidden_part, down_part, preferred_element_type=jnp.float32)
                partial_sum = partial_sum + combine[:, index:index + 1] * projected
            return total + partial_sum.astype(jnp.bfloat16).astype(jnp.float32)
        total = lax.fori_loop(0, N_FS, add_block, jnp.zeros((rows_in.shape[0], rows_in.shape[1]), jnp.float32))
        return total.astype(jnp.bfloat16)
    mixed = lax.map(one_batch, (tokens, route, route_weight))
    return (gate_out, up_out, down_out, mixed)
```

```python
import functools

import jax
import jax.numpy as jnp
from jax import lax
from jax.experimental import pallas as pl
from jax.experimental.pallas import tpu as pltpu
from jax.sharding import PartitionSpec as P

GROUP = ("gr", "tp")
MESH = pl.DeviceIdType.MESH
LANES = 128


def mixing(chosen, weights, experts):
    share = weights / jnp.sum(weights, axis=-1, keepdims=True)
    labels = jnp.arange(experts, dtype=jnp.int32)
    match = (chosen[:, :, None] == labels[None, None, :]).astype(jnp.float32)
    return jnp.sum(share[:, :, None] * match, axis=1)


def kernel(
    n_fs, side,
    tok, gate_b, up_b, down_b, comb,
    gate_o, up_o, down_o, mixed_o, stage,
    nrm, total, w1, wd, hid, bounce, dbounce, ysend, yrecv, zsend, zrecv, mout,
    x1s, x1r, z1s, z2s, rl, rs, x2s, d1s, d2s, dxs, dxr, dps, dpr, dfs, dfr, ys, yr, zs, zr, lsem,
):
    gr, s, tp = lax.axis_index("gr"), lax.axis_index("fs"), lax.axis_index("tp")
    src = (gate_b, up_b)
    out = (gate_o, up_o)
    experts, blocks, rows, width = gate_b.shape
    depth = n_fs * rows
    high = down_b.shape[2]
    count, features = tok.shape
    long = rows - side
    tile_rows = count // n_fs
    n_hi = n_fs // 2
    z, y = s // 2, s % 2

    g, other = gr * 2 + tp, (1 - gr) * 2 + tp
    home = s // blocks
    off_plane = (gr - home // 2) * (gr - home // 2)
    off_core = (tp - home % 2) * (tp - home % 2)
    receives = off_core == 0
    lo = side * off_plane
    far_lo = long * off_plane
    back_lo = long * (1 - off_plane)

    across = {"gr": 1 - gr, "fs": s, "tp": tp}
    partner = {"gr": gr, "fs": s, "tp": 1 - tp}

    def along(f):
        return {"gr": gr, "fs": f, "tp": tp}

    def remote(a, b, send, recv, to):
        return pltpu.make_async_remote_copy(
            src_ref=a, dst_ref=b, send_sem=send, recv_sem=recv, device_id=to, device_id_type=MESH
        )

    def window(start, size):
        return pl.ds(pl.multiple_of(start, 16), size)

    def x1(e, m, j):
        u = 2 * e + m
        return remote(
            src[m].at[e, j, pl.ds(side, long)], stage.at[e, m, j], x1s.at[u, j], x1r.at[u, j], across
        )

    def z1(e, m, j):
        u = 2 * e + m
        return remote(
            src[m].at[e, j, pl.ds(0, long)], out[m].at[e, window(s * rows, long)],
            z1s.at[u, j], rl.at[u, s], along(g * blocks + j),
        )

    def z2(e, m, j):
        u = 2 * e + m
        return remote(
            stage.at[e, m, j], out[m].at[e, window(s * rows + side, long)],
            z2s.at[u, j], rl.at[u, s], along(other * blocks + j),
        )

    def long_part(e, m, at):
        return out[m].at[e, window(at * rows + lo, long)]

    def d1(e, m, at):
        u = 2 * e + m
        part = long_part(e, m, at)
        return remote(part, part, d1s.at[u, at], rl.at[u, at], partner)

    def x2(e, m, at):
        u = 2 * e + m
        part = out[m].at[e, window(at * rows + far_lo, side)]
        return remote(part, part, x2s.at[u, at], rs.at[u, at], across)

    def d2(e, m, at):
        u = 2 * e + m
        part = out[m].at[e, window(at * rows + back_lo, side)]
        return remote(part, part, d2s.at[u, at], rs.at[u, at], partner)

    def columns(group):
        return pl.ds(pl.multiple_of(group * high, LANES), high)

    def dx(e):
        return remote(down_b.at[e], down_o.at[e, :, columns(g)], dxs.at[e], dxr.at[e], across)

    def dp(e):
        return remote(down_b.at[e], down_o.at[e, :, columns(g)], dps.at[e], dpr.at[e], partner)

    def df(e):
        part = down_o.at[e, :, columns(other)]
        return remote(part, part, dfs.at[e], dfr.at[e], partner)

    def each(fn):
        lax.fori_loop(0, n_fs, lambda k, c: (fn(k), c)[1], 0)

    def start_x1(e):
        for m in range(2):
            for j in range(blocks):
                x1(e, m, j).start()

    def start_z1(e):
        for m in range(2):
            for j in range(blocks):
                @pl.when(g * blocks + j != s)
                def _():
                    z1(e, m, j).start()

    def start_down(e):
        dx(e).start()
        dp(e).start()

    def relay(e):
        for m in range(2):
            for j in range(blocks):
                x1(e, m, j).wait_recv()

                @pl.when(other * blocks + j != s)
                def _():
                    z2(e, m, j).start()

    def relay_down(e):
        dx(e).wait_recv()
        df(e).start()

    def local(a, buffer, b):
        copy = pltpu.make_async_copy(a, buffer, lsem.at[0])
        copy.start()
        copy.wait()
        copy = pltpu.make_async_copy(buffer, b, lsem.at[0])
        copy.start()
        copy.wait()

    def collect_long(e):
        @pl.when(receives)
        def _():
            for m in range(2):
                mine = s - home * blocks

                @pl.when(off_plane == 0)
                def _():
                    local(src[m].at[e, mine, pl.ds(0, long)], bounce, long_part(e, m, s))

                @pl.when(off_plane != 0)
                def _():
                    local(stage.at[e, m, mine], bounce, long_part(e, m, s))

            def step(k):
                at = lax.rem(s + k, n_fs)
                for m in range(2):
                    @pl.when(k != 0)
                    def _():
                        d1(e, m, at).wait_recv()

                    x2(e, m, at).start()
                    d1(e, m, at).start()

            each(step)

    def collect_short(e):
        @pl.when(receives)
        def _():
            def step(k):
                at = lax.rem(s + k, n_fs)
                for m in range(2):
                    d2(e, m, at).wait_recv()
                    d2(e, m, at).start()

            each(step)

        @pl.when(off_core != 0)
        def _():
            def step(k):
                at = lax.rem(s + k, n_fs)
                for m in range(2):
                    d1(e, m, at).wait_recv()
                    d2(e, m, at).wait_recv()

            each(step)

    fused = width % LANES == 0

    def load(e):
        dp(e).wait_recv()
        df(e).wait_recv()
        copies = [pltpu.make_async_copy(down_o.at[e], wd, lsem.at[1])]
        if fused:
            for c in range(width // LANES):
                for m in range(2):
                    copies.append(
                        pltpu.make_async_copy(
                            out[m].at[e, :, pl.ds(c * LANES, LANES)],
                            w1.at[c, :, pl.ds(m * LANES, LANES)],
                            lsem.at[2 + 2 * c + m],
                        )
                    )
        else:
            for m in range(2):
                copies.append(pltpu.make_async_copy(out[m].at[e], w1.at[m], lsem.at[2 + m]))
        for copy in copies:
            copy.start()
        for copy in copies:
            copy.wait()

    def gated(gate_act, up_act):
        return (gate_act / (1.0 + jnp.exp(-gate_act)) * up_act).astype(jnp.bfloat16)

    def dot(a, b):
        return jnp.dot(a, b, preferred_element_type=jnp.float32)

    step_n = min(512, features)

    def tile(e, t):
        at = window(t * tile_rows, tile_rows)
        if fused:
            def hidden(c, carry):
                both = dot(nrm[at, :], w1[c])
                hid[:, pl.ds(pl.multiple_of(c * LANES, LANES), LANES)] = gated(both[:, :LANES], both[:, LANES:])
                return carry

            lax.fori_loop(0, width // LANES, hidden, 0)
        else:
            hid[...] = gated(dot(nrm[at, :], w1[0]), dot(nrm[at, :], w1[1]))

        def project(c, carry):
            cols = pl.ds(pl.multiple_of(c * step_n, LANES), step_n)
            term = comb[at, e : e + 1] * dot(hid[...], wd[:, cols])
            total[at, cols] = term if e == 0 else total[at, cols] + term
            return carry

        lax.fori_loop(0, features // step_n, project, 0)
        return at

    barrier = pltpu.get_barrier_semaphore()

    def greet(k, c):
        pl.semaphore_signal(barrier, inc=1, device_id=along(lax.rem(s + k, n_fs)), device_id_type=MESH)
        return c

    lax.fori_loop(1, n_fs, greet, 0)
    pl.semaphore_signal(barrier, inc=1, device_id=across, device_id_type=MESH)
    pl.semaphore_signal(barrier, inc=1, device_id=partner, device_id_type=MESH)
    pl.semaphore_wait(barrier, n_fs + 1)

    last = experts - 1
    start_x1(0)
    start_z1(0)
    start_down(0)
    for e in range(1, experts):
        if e < 2:
            start_x1(e)
        start_z1(e)

    fetch = pltpu.make_async_copy(tok, nrm, lsem.at[0])
    fetch.start()
    fetch.wait()

    def norm_step(t, carry):
        at = window(t * tile_rows, tile_rows)
        values = nrm[at, :].astype(jnp.float32)
        mean = jnp.mean(values * values, axis=-1, keepdims=True)
        nrm[at, :] = (values * lax.rsqrt(mean + 1e-06)).astype(jnp.bfloat16)
        return carry

    lax.fori_loop(0, n_fs, norm_step, 0)
    for e in range(experts):
        local(down_b.at[e], dbounce, down_o.at[e, :, columns(g)])

    relay(0)
    for e in range(experts):
        collect_long(e)
        if e + 2 < experts:
            start_x1(e + 2)
        if e + 1 < experts:
            start_down(e + 1)
            relay(e + 1)
        relay_down(e)
        collect_short(e)
        load(e)
        if e < last:
            each(lambda t, e=e: tile(e, t))

    def to_pair(k):
        zt = lax.rem(z + 1 + k, n_hi)
        return remote(ysend.at[k], yrecv.at[zt], ys.at[k], yr.at[zt], along(s + 1 - 2 * y))

    def to_owner(k):
        zt = lax.rem(z + 1 + k, n_hi)
        return remote(zsend.at[k], zrecv.at[k], zs.at[k], zr.at[k], along(zt * 2 + y))

    def pair_step(k, carry):
        zt = lax.rem(z + 1 + k, n_hi)
        at = tile(last, zt * 2 + 1 - y)
        ysend[k] = total[at, :].astype(jnp.bfloat16)
        to_pair(k).start()
        return carry

    lax.fori_loop(0, n_hi, pair_step, 0)

    def owner_step(k, carry):
        zt = lax.rem(z + 1 + k, n_hi)
        at = tile(last, zt * 2 + y)
        remote(ysend.at[k], yrecv.at[zt], ys.at[k], yr.at[zt], along(s + 1 - 2 * y)).wait_recv()
        zsend[k] = (total[at, :] + yrecv[zt].astype(jnp.float32)).astype(jnp.bfloat16)
        to_owner(k).start()
        return carry

    lax.fori_loop(0, n_hi - 1, owner_step, 0)
    at = tile(last, s)
    to_pair(n_hi - 1).wait_recv()
    total[at, :] = total[at, :] + yrecv[z].astype(jnp.float32)

    def gather_step(k, carry):
        to_owner(k).wait_recv()
        total[at, :] = total[at, :] + zrecv[k].astype(jnp.float32)
        return carry

    lax.fori_loop(0, n_hi - 1, gather_step, 0)
    mout[...] = total[at, :].astype(jnp.bfloat16)
    done = pltpu.make_async_copy(mout, mixed_o, lsem.at[0])
    done.start()
    done.wait()

    for e in range(experts):
        dx(e).wait_send()
        dp(e).wait_send()
        df(e).wait_send()
        for m in range(2):
            for j in range(blocks):
                x1(e, m, j).wait_send()

                @pl.when(g * blocks + j != s)
                def _():
                    z1(e, m, j).wait_send()

                @pl.when(other * blocks + j != s)
                def _():
                    z2(e, m, j).wait_send()

            @pl.when(receives)
            def _():
                def step(k):
                    x2(e, m, k).wait_send()
                    d1(e, m, k).wait_send()
                    d2(e, m, k).wait_send()

                each(step)

    def drain_pair(k, carry):
        to_pair(k).wait_send()
        return carry

    def drain_owner(k, carry):
        to_owner(k).wait_send()
        return carry

    lax.fori_loop(0, n_hi, drain_pair, 0)
    lax.fori_loop(0, n_hi - 1, drain_owner, 0)


def make_shards(n_fs, n_group):
    def shards(tokens, gate_master, up_master, down_master, norm_gain, route, route_weight):
        experts, rows, columns = gate_master.shape
        blocks = n_fs // n_group
        width = columns // blocks
        depth = rows * n_fs
        _, count, features = tokens.shape
        high = down_master.shape[2]
        side = 16 * max(1, round(rows / 96))
        long = rows - side
        tile_rows = count // n_fs
        n_hi = n_fs // 2
        units = 2 * experts

        def cut(master):
            scaled = (norm_gain[None, :, None] * master).astype(jnp.bfloat16)
            return scaled.reshape(experts, rows, blocks, width).transpose(0, 2, 1, 3)

        gate_b, up_b = cut(gate_master), cut(up_master)
        down_b = down_master.astype(jnp.bfloat16)
        comb = mixing(route[0], route_weight[0], experts)
        bf16 = jnp.bfloat16
        fused = width % LANES == 0
        parts = width // LANES if fused else 2
        anywhere = pl.BlockSpec(memory_space=pl.ANY)
        dma = pltpu.SemaphoreType.DMA
        gate_out, up_out, down_out, mixed, _ = pl.pallas_call(
            functools.partial(kernel, n_fs, side),
            out_shape=(
                jax.ShapeDtypeStruct((experts, depth, width), bf16),
                jax.ShapeDtypeStruct((experts, depth, width), bf16),
                jax.ShapeDtypeStruct((experts, width, n_group * high), bf16),
                jax.ShapeDtypeStruct((tile_rows, features), bf16),
                jax.ShapeDtypeStruct((experts, 2, blocks, long, width), bf16),
            ),
            in_specs=[anywhere] * 4 + [pl.BlockSpec(memory_space=pltpu.VMEM)],
            out_specs=[anywhere] * 5,
            scratch_shapes=[
                pltpu.VMEM((count, features), bf16),
                pltpu.VMEM((count, features), jnp.float32),
                pltpu.VMEM((parts, depth, 2 * LANES if fused else width), bf16),
                pltpu.VMEM((width, features), bf16),
                pltpu.VMEM((tile_rows, width), bf16),
                pltpu.VMEM((long, width), bf16),
                pltpu.VMEM((width, high), bf16),
                pltpu.VMEM((n_hi, tile_rows, features), bf16),
                pltpu.VMEM((n_hi, tile_rows, features), bf16),
                pltpu.VMEM((n_hi - 1, tile_rows, features), bf16),
                pltpu.VMEM((n_hi - 1, tile_rows, features), bf16),
                pltpu.VMEM((tile_rows, features), bf16),
                dma((units, blocks)), dma((units, blocks)), dma((units, blocks)), dma((units, blocks)),
                dma((units, n_fs)), dma((units, n_fs)), dma((units, n_fs)), dma((units, n_fs)), dma((units, n_fs)),
                dma((experts,)), dma((experts,)), dma((experts,)), dma((experts,)), dma((experts,)), dma((experts,)),
                dma((n_hi,)), dma((n_hi,)), dma((n_hi,)), dma((n_hi,)),
                dma((2 + 2 * parts,)),
            ],
            compiler_params=pltpu.CompilerParams(
                collective_id=0, has_side_effects=True, vmem_limit_bytes=67043328
            ),
        )(tokens[0], gate_b, up_b, down_b, comb)
        return gate_out, up_out, down_out, mixed[None]

    return shards


def solution(mesh):
    n_fs = mesh.shape["fs"]
    n_group = mesh.shape["gr"] * mesh.shape["tp"]
    in_specs = (
        P(GROUP, None, None),
        P(None, "fs", GROUP),
        P(None, "fs", GROUP),
        P(None, "fs", GROUP),
        P("fs"),
        P(GROUP, None, None),
        P(GROUP, None, None),
    )
    out_specs = (
        P(None, None, "fs"),
        P(None, None, "fs"),
        P(None, "fs", None),
        P(GROUP, "fs", None),
    )
    return jax.shard_map(
        make_shards(n_fs, n_group), mesh=mesh, in_specs=in_specs, out_specs=out_specs, check_vma=False
    )
```

```python
import functools

import jax
import jax.numpy as jnp
from jax import lax
from jax.experimental import pallas as pl
from jax.experimental.pallas import tpu as pltpu
from jax.sharding import PartitionSpec as P

GROUP = ("gr", "tp")
MESH = pl.DeviceIdType.MESH
LANES = 128


def mixing(chosen, weights, experts):
    labels = jnp.arange(experts, dtype=jnp.int32)[None, :]
    total = weights[:, :1] + weights[:, 1:2]
    first = jnp.where(chosen[:, :1] == labels, weights[:, :1] / total, 0.0)
    second = jnp.where(chosen[:, 1:2] == labels, weights[:, 1:2] / total, 0.0)
    return first + second


def kernel(
    n_fs, sides,
    tok, gate_m, up_m, down_m, gain, comb,
    gate_o, up_o, down_o, mixed_o, stage, gate_b, up_b, down_b,
    nrm, total, w1, wd, hid, bounce, dstage, dbounce, cast, ysend, yrecv, zsend, zrecv, mout,
    x1s, x1r, z1s, z2s, rl, rs, x2s, d1s, d2s, dxs, dxr, dps, dpr, dfs, dfr, ys, yr, zs, zr, lsem, msem, wsem, dsem,
):
    gr, s, tp = lax.axis_index("gr"), lax.axis_index("fs"), lax.axis_index("tp")
    src = (gate_b, up_b)
    masters = (gate_m, up_m)
    out = (gate_o, up_o)
    experts, blocks, rows, width = gate_b.shape
    depth = n_fs * rows
    high = down_b.shape[2]
    count, features = tok.shape
    longs_of = [rows - side for side in sides]
    tile_rows = count // n_fs
    n_hi = n_fs // 2
    z, y = s // 2, s % 2

    g, other = gr * 2 + tp, (1 - gr) * 2 + tp
    home = s // blocks
    off_plane = (gr - home // 2) * (gr - home // 2)
    off_core = (tp - home % 2) * (tp - home % 2)
    receives = off_core == 0

    across = {"gr": 1 - gr, "fs": s, "tp": tp}
    partner = {"gr": gr, "fs": s, "tp": 1 - tp}
    relayer = {"gr": 1 - gr, "fs": s, "tp": 1 - home % 2}

    def along(f, core=tp):
        return {"gr": gr, "fs": f, "tp": core}

    def remote(a, b, send, recv, to):
        return pltpu.make_async_remote_copy(
            src_ref=a, dst_ref=b, send_sem=send, recv_sem=recv, device_id=to, device_id_type=MESH
        )

    def window(start, size):
        return pl.ds(pl.multiple_of(start, 16), size)

    def staged(e, m, j, core):
        return stage.at[core, e, m, j, pl.ds(0, longs_of[e])]

    def x1(e, m, j, core=tp):
        u = 2 * e + m
        return remote(
            src[m].at[e, j, pl.ds(sides[e], longs_of[e])], staged(e, m, j, core), x1s.at[u, j], x1r.at[core, u, j], relayer
        )

    def z1(e, m, j):
        u = 2 * e + m
        return remote(
            src[m].at[e, j, pl.ds(0, longs_of[e])], out[m].at[e, window(s * rows, longs_of[e])],
            z1s.at[u, j], rl.at[u, s], along(g * blocks + j),
        )

    def z2(e, m, j, core):
        u = 2 * e + m
        at = ((1 - gr) * 2 + core) * blocks + j
        return remote(
            staged(e, m, j, core), out[m].at[e, window(s * rows + sides[e], longs_of[e])],
            z2s.at[core, u, j], rl.at[u, s], along(at, core),
        )

    def long_part(e, m, at):
        return out[m].at[e, window(at * rows + sides[e] * off_plane, longs_of[e])]

    def d1(e, m, at):
        u = 2 * e + m
        part = long_part(e, m, at)
        return remote(part, part, d1s.at[u, at], rl.at[u, at], partner)

    def x2(e, m, at):
        u = 2 * e + m
        part = out[m].at[e, window(at * rows + longs_of[e] * off_plane, sides[e])]
        return remote(part, part, x2s.at[u, at], rs.at[u, at], across)

    def d2(e, m, at):
        u = 2 * e + m
        part = out[m].at[e, window(at * rows + longs_of[e] * (1 - off_plane), sides[e])]
        return remote(part, part, d2s.at[u, at], rs.at[u, at], partner)

    def columns(group):
        return pl.ds(pl.multiple_of(group * high, LANES), high)

    def dx(e):
        return remote(down_b.at[e], down_o.at[e, :, columns(g)], dxs.at[e], dxr.at[e], across)

    def dp(e):
        return remote(down_b.at[e], down_o.at[e, :, columns(g)], dps.at[e], dpr.at[e], partner)

    def df(e):
        part = down_o.at[e, :, columns(other)]
        return remote(part, part, dfs.at[e], dfr.at[e], partner)

    def each(fn):
        lax.fori_loop(0, n_fs, lambda k, c: (fn(k), c)[1], 0)

    def start_x1(e):
        for m in range(2):
            for j in range(blocks):
                x1(e, m, j).start()

    def start_down(e):
        dx(e).start()
        dp(e).start()

    def relay(e):
        for m in range(2):
            for j in range(blocks):
                for core in range(2):
                    x1(e, m, j, core).wait_recv()
                    z2(e, m, j, core).start()

    def relay_down(e):
        dx(e).wait_recv()
        df(e).start()

    def local(a, buffer, b):
        copy = pltpu.make_async_copy(a, buffer, lsem.at[0])
        copy.start()
        copy.wait()
        copy = pltpu.make_async_copy(buffer, b, lsem.at[0])
        copy.start()
        copy.wait()

    def long_step(e, k):
        at = lax.rem(s + k, n_fs)
        near = off_plane + k == 0
        for m in range(2):
            @pl.when(near)
            def _():
                local(
                    src[m].at[e, s - home * blocks, pl.ds(0, longs_of[e])],
                    bounce.at[pl.ds(0, longs_of[e])],
                    long_part(e, m, s),
                )

            @pl.when(jnp.logical_not(near))
            def _():
                d1(e, m, at).wait_recv()

            x2(e, m, at).start()
            d1(e, m, at).start()

    def short_step(e, k):
        at = lax.rem(s + k, n_fs)
        for m in range(2):
            d2(e, m, at).wait_recv()
            d2(e, m, at).start()

    def final_step(e, k):
        at = lax.rem(s + k, n_fs)
        for m in range(2):
            d1(e, m, at).wait_recv()
            d2(e, m, at).wait_recv()

    fused = width % LANES == 0

    def load(e):
        dp(e).wait_recv()
        df(e).wait_recv()
        copies = [pltpu.make_async_copy(down_o.at[e], wd, lsem.at[1])]
        if fused:
            for c in range(width // LANES):
                for m in range(2):
                    copies.append(
                        pltpu.make_async_copy(
                            out[m].at[e, :, pl.ds(c * LANES, LANES)],
                            w1.at[c, :, pl.ds(m * LANES, LANES)],
                            lsem.at[2 + 2 * c + m],
                        )
                    )
        else:
            for m in range(2):
                copies.append(pltpu.make_async_copy(out[m].at[e], w1.at[m], lsem.at[2 + m]))
        for copy in copies:
            copy.start()
        for copy in copies:
            copy.wait()

    def gated(gate_act, up_act):
        return (gate_act / (1.0 + jnp.exp(-gate_act)) * up_act).astype(jnp.bfloat16)

    def dot(a, b):
        return jnp.dot(a, b, preferred_element_type=jnp.float32)

    step_n = min(512, features)

    def tile(e, start, size, flat=False):
        at = window(start, size)
        rows_of = pl.ds(0, size)
        if fused:
            def hidden(c, carry):
                both = dot(nrm[at, :], w1[c])
                cols = pl.ds(pl.multiple_of(c * LANES, LANES), LANES)
                hid[rows_of, cols] = gated(both[:, :LANES], both[:, LANES:])
                return carry

            lax.fori_loop(0, width // LANES, hidden, 0, unroll=flat)
        else:
            hid[rows_of, :] = gated(dot(nrm[at, :], w1[0]), dot(nrm[at, :], w1[1]))

        def project(c, carry):
            cols = pl.ds(pl.multiple_of(c * step_n, LANES), step_n)
            term = comb[at, e : e + 1] * dot(hid[rows_of, :], wd[:, cols])
            total[at, cols] = term if e == 0 else total[at, cols] + term
            return carry

        lax.fori_loop(0, features // step_n, project, 0, unroll=flat)
        return at

    def read(u):
        return pltpu.make_async_copy(
            masters[u % 2].at[u // 2],
            total.at[pl.ds(u * rows, rows), pl.ds(0, blocks * width)],
            msem.at[u],
        )

    def write(u):
        return pltpu.make_async_copy(cast.at[u % 2], src[u % 2].at[u // 2], wsem.at[u % 2])

    def read_down(e):
        return pltpu.make_async_copy(down_m.at[e], dstage, dsem.at[0])

    def write_down(e):
        return (
            pltpu.make_async_copy(dbounce, down_b.at[e], dsem.at[1]),
            pltpu.make_async_copy(dbounce, down_o.at[e, :, columns(g)], dsem.at[2]),
        )

    def round_unit(u):
        read(u).wait()
        for j in range(blocks):
            part = total[pl.ds(u * rows, rows), j * width : (j + 1) * width]
            cast[u % 2, j] = (gain[...] * part).astype(jnp.bfloat16)
        write(u).start()

    def start_z1(e, m):
        for j in range(blocks):
            @pl.when(g * blocks + j != s)
            def _():
                z1(e, m, j).start()

    def release(u):
        e, m = u // 2, u % 2
        write(u).wait()
        for j in range(blocks):
            x1(e, m, j).start()
        if e == 0:
            start_z1(e, m)

    def round_down(e):
        read_down(e).wait()
        dbounce[...] = dstage[...].astype(jnp.bfloat16)
        for copy in write_down(e):
            copy.start()
        if e + 1 < experts:
            read_down(e + 1).start()
        for copy in write_down(e):
            copy.wait()

    units = 2 * experts
    for u in range(units):
        read(u).start()
    read_down(0).start()
    barrier = pltpu.get_barrier_semaphore()

    def hello(to):
        pl.semaphore_signal(barrier, inc=1, device_id=to, device_id_type=MESH)

    def greet(k, c):
        at = lax.rem(s + k, n_fs)
        hello(along(at))
        hello(along(at, 1 - tp))
        return c

    lax.fori_loop(1, n_fs, greet, 0)
    hello(partner)
    hello(across)
    hello({"gr": 1 - gr, "fs": s, "tp": 1 - tp})
    pl.semaphore_wait(barrier, 2 * n_fs + 1)

    last = experts - 1
    fetch = pltpu.make_async_copy(tok, nrm, lsem.at[0])
    fetch.start()
    early = min(2, experts)
    with jax.named_scope("cast"):
        for u in range(2 * early):
            round_unit(u)
            if u >= 1:
                release(u - 1)
        release(2 * early - 1)
        round_down(0)
        start_down(0)

    def norm_step(t, carry):
        at = window(t * tile_rows, tile_rows)
        values = nrm[at, :].astype(jnp.float32)
        mean = jnp.mean(values * values, axis=-1, keepdims=True)
        nrm[at, :] = (values * lax.rsqrt(mean + 1e-06)).astype(jnp.bfloat16)
        return carry

    def late():
        with jax.named_scope("late"):
            for u in range(2 * early, units):
                round_unit(u)
                write(u).wait()
            for e in range(1, experts):
                round_down(e)
            fetch.wait()
            lax.fori_loop(0, n_fs, norm_step, 0)

    big = 2 * tile_rows

    def more_x(e):
        if e + 2 < experts:
            start_x1(e + 2)

    def more_down(e):
        if e + 1 < experts:
            start_down(e + 1)

    def open_z(e):
        if 0 < e < experts:
            for m in range(2):
                start_z1(e, m)

    def longs(e, start, stop):
        with jax.named_scope(f"long{e}"):
            lax.fori_loop(start, stop, lambda k, c: (long_step(e, k), c)[1], 0)

    def shorts(e):
        with jax.named_scope(f"rdown{e}"):
            relay_down(e)
        with jax.named_scope(f"short{e}"):
            each(lambda k: short_step(e, k))

    half_fs = n_fs // 2
    for e in range(experts):
        @pl.when(receives)
        def _(e=e):
            if e == 0:
                late()
                open_z(1)
                longs(0, 0, half_fs)
                longs(0, half_fs, n_fs)
                more_x(0)
                more_down(0)
                open_z(2)
                if experts > 2:
                    longs(1, 0, half_fs)
            shorts(e)
            if e == 0:
                if experts > 2:
                    longs(1, half_fs, n_fs)
            else:
                more_x(e)
                more_down(e)
                open_z(e + 2)

        @pl.when(off_core != 0)
        def _(e=e):
            if e == 0:
                for ahead in range(experts):
                    with jax.named_scope(f"relay{ahead}"):
                        relay(ahead)
                    if ahead == 0:
                        open_z(1)
                        late()
                    else:
                        if ahead == 1:
                            with jax.named_scope("rdown0"):
                                relay_down(0)
                        open_z(ahead + 1)
                    more_x(ahead)
                    if ahead == 0:
                        more_down(0)
            else:
                more_down(e)
                with jax.named_scope(f"rdown{e}"):
                    relay_down(e)
            with jax.named_scope(f"final{e}"):
                each(lambda k: final_step(e, k))

        with jax.named_scope(f"load{e}"):
            load(e)
        if e < last:
            follow = e + 1 if experts == 2 or e > 0 else experts

            def both(t, carry, e=e, follow=follow):
                tile(e, t * big, big, True)
                if follow < experts:
                    @pl.when(receives)
                    def _():
                        long_step(follow, 2 * t)
                        long_step(follow, 2 * t + 1)

                return carry

            with jax.named_scope(f"dots{e}"):
                lax.fori_loop(0, half_fs, both, 0)

    half = n_hi // 2
    upper = z // half
    step_h = features // 2

    def turn(k):
        crossing = 1 - k // half
        return (upper + crossing * (1 - 2 * upper)) * half + (z + 1 + k) % half

    def to_pair(k, h):
        zt = turn(k)
        return remote(ysend.at[k, h], yrecv.at[zt, h], ys.at[k, h], yr.at[zt, h], along(s + 1 - 2 * y))

    def to_owner(k, h, cross=False):
        zt = (1 - upper) * half + z % half if cross else upper * half + (z + 1 + k) % half
        return remote(zsend.at[k, h], zrecv.at[k, h], zs.at[k, h], zr.at[k, h], along(zt * 2 + y))

    def pair_step(k, carry):
        at = tile(last, (turn(k) * 2 + 1 - y) * tile_rows, tile_rows)
        for h in range(2):
            ysend[k, h] = total[at, h * step_h : (h + 1) * step_h].astype(jnp.bfloat16)
            to_pair(k, h).start()
        return carry

    def summed(at, k, h):
        to_pair(k, h).wait_recv()
        return total[at, h * step_h : (h + 1) * step_h] + yrecv[turn(k), h].astype(jnp.float32)

    def drain_weights():
        for e in range(experts):
            dx(e).wait_send()
            dp(e).wait_send()
            df(e).wait_send()
            for m in range(2):
                for j in range(blocks):
                    x1(e, m, j).wait_send()

                    @pl.when(g * blocks + j != s)
                    def _():
                        z1(e, m, j).wait_send()

                    @pl.when(off_core != 0)
                    def _():
                        for core in range(2):
                            z2(e, m, j, core).wait_send()

                @pl.when(receives)
                def _():
                    def step(k):
                        x2(e, m, k).wait_send()
                        d1(e, m, k).wait_send()
                        d2(e, m, k).wait_send()

                    each(step)

    def halves(h):
        return slice(h * step_h, (h + 1) * step_h)

    def add_arrived(at, h, start, stop):
        def step(k, carry):
            to_owner(k, h).wait_recv()
            total[at, halves(h)] = total[at, halves(h)] + zrecv[k, h].astype(jnp.float32)
            return carry

        lax.fori_loop(start, stop, step, 0)

    def owner_step(k, cross):
        at = tile(last, (turn(k) * 2 + y) * tile_rows, tile_rows)
        for h in range(2):
            if cross:
                total[at, halves(h)] = summed(at, k, h)
                add_arrived(at, h, 0, half - 1)
                zsend[k, h] = total[at, halves(h)].astype(jnp.bfloat16)
            else:
                zsend[k, h] = summed(at, k, h).astype(jnp.bfloat16)
            to_owner(k, h, cross).start()

    def owners(start, stop, cross, lead):
        def step(k, carry):
            if lead:
                pair_step(k + lead, carry)
            owner_step(k, cross)
            return carry

        if stop > start:
            lax.fori_loop(start, stop, step, 0)

    lead = min(2, n_hi - half)
    with jax.named_scope("pairs"):
        lax.fori_loop(0, lead, pair_step, 0)
    with jax.named_scope("owners"):
        owners(0, half - 1, False, lead)
        owners(half - 1, half, True, lead)
        owners(half, n_hi - lead, False, lead)
        owners(n_hi - lead, n_hi - 1, False, 0)
    drain_weights()
    with jax.named_scope("own"):
        at = tile(last, s * tile_rows, tile_rows)
        for h in range(2):
            total[at, halves(h)] = summed(at, n_hi - 1, h)
            add_arrived(at, h, half - 1, n_hi - 1)
    mout[...] = total[at, :].astype(jnp.bfloat16)
    done = pltpu.make_async_copy(mout, mixed_o, lsem.at[0])
    done.start()
    done.wait()

    def drain_pair(k, carry):
        for h in range(2):
            to_pair(k, h).wait_send()
        return carry

    def drain_owner(k, carry):
        for h in range(2):
            to_owner(k, h).wait_send()
        return carry

    lax.fori_loop(0, n_hi, drain_pair, 0)
    lax.fori_loop(0, n_hi - 1, drain_owner, 0)


def make_shards(n_fs, n_group):
    def shards(tokens, gate_master, up_master, down_master, norm_gain, route, route_weight):
        experts, rows, columns = gate_master.shape
        blocks = n_fs // n_group
        width = columns // blocks
        depth = rows * n_fs
        _, count, features = tokens.shape
        high = down_master.shape[2]
        shares = (4, 6) + (2,) * experts
        sides = tuple(16 * max(1, rows * shares[e] // 256) for e in range(experts))
        long = rows - min(sides)
        tile_rows = count // n_fs
        n_hi = n_fs // 2
        units = 2 * experts

        comb = mixing(route[0], route_weight[0], experts)
        bf16 = jnp.bfloat16
        fused = width % LANES == 0
        parts = width // LANES if fused else 2
        anywhere = pl.BlockSpec(memory_space=pl.ANY)
        dma = pltpu.SemaphoreType.DMA
        gate_out, up_out, down_out, mixed, *_ = pl.pallas_call(
            functools.partial(kernel, n_fs, sides),
            out_shape=(
                jax.ShapeDtypeStruct((experts, depth, width), bf16),
                jax.ShapeDtypeStruct((experts, depth, width), bf16),
                jax.ShapeDtypeStruct((experts, width, n_group * high), bf16),
                jax.ShapeDtypeStruct((tile_rows, features), bf16),
                jax.ShapeDtypeStruct((2, experts, 2, blocks, long, width), bf16),
                jax.ShapeDtypeStruct((experts, blocks, rows, width), bf16),
                jax.ShapeDtypeStruct((experts, blocks, rows, width), bf16),
                jax.ShapeDtypeStruct((experts, width, high), bf16),
            ),
            in_specs=[anywhere] * 4 + [pl.BlockSpec(memory_space=pltpu.VMEM)] * 2,
            out_specs=[anywhere] * 8,
            scratch_shapes=[
                pltpu.VMEM((count, features), bf16),
                pltpu.VMEM((count, features), jnp.float32),
                pltpu.VMEM((parts, depth, 2 * LANES if fused else width), bf16),
                pltpu.VMEM((width, features), bf16),
                pltpu.VMEM((2 * tile_rows, width), bf16),
                pltpu.VMEM((long, width), bf16),
                pltpu.VMEM((width, high), jnp.float32),
                pltpu.VMEM((width, high), bf16),
                pltpu.VMEM((2, blocks, rows, width), bf16),
                pltpu.VMEM((n_hi, 2, tile_rows, features // 2), bf16),
                pltpu.VMEM((n_hi, 2, tile_rows, features // 2), bf16),
                pltpu.VMEM((n_hi - 1, 2, tile_rows, features // 2), bf16),
                pltpu.VMEM((n_hi - 1, 2, tile_rows, features // 2), bf16),
                pltpu.VMEM((tile_rows, features), bf16),
                dma((units, blocks)), dma((2, units, blocks)), dma((units, blocks)), dma((2, units, blocks)),
                dma((units, n_fs)), dma((units, n_fs)), dma((units, n_fs)), dma((units, n_fs)), dma((units, n_fs)),
                dma((experts,)), dma((experts,)), dma((experts,)), dma((experts,)), dma((experts,)), dma((experts,)),
                dma((n_hi, 2)), dma((n_hi, 2)), dma((n_hi, 2)), dma((n_hi, 2)),
                dma((2 + 2 * parts,)), dma((units,)), dma((2,)), dma((3,)),
            ],
            compiler_params=pltpu.CompilerParams(
                collective_id=0, has_side_effects=True, vmem_limit_bytes=67043328
            ),
        )(tokens[0], gate_master, up_master, down_master, norm_gain[:, None], comb)
        return gate_out, up_out, down_out, mixed[None]

    return shards


def solution(mesh):
    n_fs = mesh.shape["fs"]
    n_group = mesh.shape["gr"] * mesh.shape["tp"]
    in_specs = (
        P(GROUP, None, None),
        P(None, "fs", GROUP),
        P(None, "fs", GROUP),
        P(None, "fs", GROUP),
        P("fs"),
        P(GROUP, None, None),
        P(GROUP, None, None),
    )
    out_specs = (
        P(None, None, "fs"),
        P(None, None, "fs"),
        P(None, "fs", None),
        P(GROUP, "fs", None),
    )
    return jax.shard_map(
        make_shards(n_fs, n_group), mesh=mesh, in_specs=in_specs, out_specs=out_specs, check_vma=False
    )
```

```python
import functools

import jax
import jax.numpy as jnp
from jax import lax
from jax.experimental import pallas as pl
from jax.experimental.pallas import tpu as pltpu
from jax.sharding import PartitionSpec as P

GROUP = ("gr", "tp")
MESH = pl.DeviceIdType.MESH
LANES = 128


def kernel(
    n_fs, sides,
    tok, gate_m, up_m, down_m, gain_row, route, weight,
    gate_o, up_o, down_o, mixed_o, stage, gate_b, up_b, down_b,
    gain, comb, nrm, total, w1, wd, hid, bounce, dstage, dbounce, cast, ysend, yrecv, zsend, zrecv, mout,
    x1s, x1r, z1s, z2s, rl, rs, x2s, d1s, d2s, dxs, dxr, dps, dpr, dfs, dfr, ys, yr, zs, zr, lsem, msem, wsem, dsem,
):
    gr, s, tp = lax.axis_index("gr"), lax.axis_index("fs"), lax.axis_index("tp")
    src = (gate_b, up_b)
    masters = (gate_m, up_m)
    out = (gate_o, up_o)
    experts, blocks, rows, width = gate_b.shape
    depth = n_fs * rows
    high = down_b.shape[2]
    count, features = tok.shape
    longs_of = [rows - side for side in sides]
    tile_rows = count // n_fs
    n_hi = n_fs // 2
    z, y = s // 2, s % 2

    g, other = gr * 2 + tp, (1 - gr) * 2 + tp
    home = s // blocks
    off_plane = (gr - home // 2) * (gr - home // 2)
    off_core = (tp - home % 2) * (tp - home % 2)
    receives = off_core == 0

    across = {"gr": 1 - gr, "fs": s, "tp": tp}
    partner = {"gr": gr, "fs": s, "tp": 1 - tp}
    relayer = {"gr": 1 - gr, "fs": s, "tp": 1 - home % 2}

    def along(f, core=tp):
        return {"gr": gr, "fs": f, "tp": core}

    def remote(a, b, send, recv, to):
        return pltpu.make_async_remote_copy(
            src_ref=a, dst_ref=b, send_sem=send, recv_sem=recv, device_id=to, device_id_type=MESH
        )

    def window(start, size):
        return pl.ds(pl.multiple_of(start, 16), size)

    def staged(e, m, j, core):
        return stage.at[core, e, m, j, pl.ds(0, longs_of[e])]

    def x1(e, m, j, core=tp):
        u = 2 * e + m
        return remote(
            src[m].at[e, j, pl.ds(sides[e], longs_of[e])], staged(e, m, j, core), x1s.at[u, j], x1r.at[core, u, j], relayer
        )

    def z1(e, m, j):
        u = 2 * e + m
        return remote(
            src[m].at[e, j, pl.ds(0, longs_of[e])], out[m].at[e, window(s * rows, longs_of[e])],
            z1s.at[u, j], rl.at[u, s], along(g * blocks + j),
        )

    def z2(e, m, j, core):
        u = 2 * e + m
        at = ((1 - gr) * 2 + core) * blocks + j
        return remote(
            staged(e, m, j, core), out[m].at[e, window(s * rows + sides[e], longs_of[e])],
            z2s.at[core, u, j], rl.at[u, s], along(at, core),
        )

    def long_part(e, m, at):
        return out[m].at[e, window(at * rows + sides[e] * off_plane, longs_of[e])]

    def d1(e, m, at):
        u = 2 * e + m
        part = long_part(e, m, at)
        return remote(part, part, d1s.at[u, at], rl.at[u, at], partner)

    def x2(e, m, at):
        u = 2 * e + m
        part = out[m].at[e, window(at * rows + longs_of[e] * off_plane, sides[e])]
        return remote(part, part, x2s.at[u, at], rs.at[u, at], across)

    def d2(e, m, at):
        u = 2 * e + m
        part = out[m].at[e, window(at * rows + longs_of[e] * (1 - off_plane), sides[e])]
        return remote(part, part, d2s.at[u, at], rs.at[u, at], partner)

    def columns(group):
        return pl.ds(pl.multiple_of(group * high, LANES), high)

    def dx(e):
        return remote(down_b.at[e], down_o.at[e, :, columns(g)], dxs.at[e], dxr.at[e], across)

    def dp(e):
        return remote(down_b.at[e], down_o.at[e, :, columns(g)], dps.at[e], dpr.at[e], partner)

    def df(e):
        part = down_o.at[e, :, columns(other)]
        return remote(part, part, dfs.at[e], dfr.at[e], partner)

    def each(fn):
        lax.fori_loop(0, n_fs, lambda k, c: (fn(k), c)[1], 0)

    def start_x1(e):
        for m in range(2):
            for j in range(blocks):
                x1(e, m, j).start()

    def start_down(e):
        dx(e).start()
        dp(e).start()

    def relay(e):
        for m in range(2):
            for j in range(blocks):
                for core in range(2):
                    x1(e, m, j, core).wait_recv()
                    z2(e, m, j, core).start()

    def relay_down(e):
        dx(e).wait_recv()
        df(e).start()

    def local(a, buffer, b):
        copy = pltpu.make_async_copy(a, buffer, lsem.at[0])
        copy.start()
        copy.wait()
        copy = pltpu.make_async_copy(buffer, b, lsem.at[0])
        copy.start()
        copy.wait()

    def long_step(e, k):
        at = lax.rem(s + k, n_fs)
        near = off_plane + k == 0
        for m in range(2):
            @pl.when(near)
            def _():
                local(
                    src[m].at[e, s - home * blocks, pl.ds(0, longs_of[e])],
                    bounce.at[pl.ds(0, longs_of[e])],
                    long_part(e, m, s),
                )

            @pl.when(jnp.logical_not(near))
            def _():
                d1(e, m, at).wait_recv()

            x2(e, m, at).start()
            d1(e, m, at).start()

    def short_step(e, k):
        at = lax.rem(s + k, n_fs)
        for m in range(2):
            d2(e, m, at).wait_recv()
            d2(e, m, at).start()

    def final_step(e, k):
        at = lax.rem(s + k, n_fs)
        for m in range(2):
            d1(e, m, at).wait_recv()
            d2(e, m, at).wait_recv()

    fused = width % LANES == 0

    def load(e):
        dp(e).wait_recv()
        df(e).wait_recv()
        copies = [pltpu.make_async_copy(down_o.at[e], wd, lsem.at[1])]
        if fused:
            for c in range(width // LANES):
                for m in range(2):
                    copies.append(
                        pltpu.make_async_copy(
                            out[m].at[e, :, pl.ds(c * LANES, LANES)],
                            w1.at[c, :, pl.ds(m * LANES, LANES)],
                            lsem.at[2 + 2 * c + m],
                        )
                    )
        else:
            for m in range(2):
                copies.append(pltpu.make_async_copy(out[m].at[e], w1.at[m], lsem.at[2 + m]))
        for copy in copies:
            copy.start()
        for copy in copies:
            copy.wait()

    def gated(gate_act, up_act):
        return (gate_act / (1.0 + jnp.exp(-gate_act)) * up_act).astype(jnp.bfloat16)

    def dot(a, b):
        return jnp.dot(a, b, preferred_element_type=jnp.float32)

    step_n = min(512, features)

    def tile(e, start, size, flat=False):
        at = window(start, size)
        rows_of = pl.ds(0, size)
        if fused:
            def hidden(c, carry):
                both = dot(nrm[at, :], w1[c])
                cols = pl.ds(pl.multiple_of(c * LANES, LANES), LANES)
                hid[rows_of, cols] = gated(both[:, :LANES], both[:, LANES:])
                return carry

            lax.fori_loop(0, width // LANES, hidden, 0, unroll=flat)
        else:
            hid[rows_of, :] = gated(dot(nrm[at, :], w1[0]), dot(nrm[at, :], w1[1]))

        def project(c, carry):
            cols = pl.ds(pl.multiple_of(c * step_n, LANES), step_n)
            term = comb[at, e : e + 1] * dot(hid[rows_of, :], wd[:, cols])
            total[at, cols] = term if e == 0 else total[at, cols] + term
            return carry

        lax.fori_loop(0, features // step_n, project, 0, unroll=flat)
        return at

    def read(u):
        return pltpu.make_async_copy(
            masters[u % 2].at[u // 2],
            total.at[pl.ds(u * rows, rows), pl.ds(0, blocks * width)],
            msem.at[u],
        )

    def write(u):
        return pltpu.make_async_copy(cast.at[u % 2], src[u % 2].at[u // 2], wsem.at[u % 2])

    def read_down(e):
        return pltpu.make_async_copy(down_m.at[e], dstage, dsem.at[0])

    def write_down(e):
        return (
            pltpu.make_async_copy(dbounce, down_b.at[e], dsem.at[1]),
            pltpu.make_async_copy(dbounce, down_o.at[e, :, columns(g)], dsem.at[2]),
        )

    def round_unit(u):
        read(u).wait()
        for j in range(blocks):
            part = total[pl.ds(u * rows, rows), j * width : (j + 1) * width]
            cast[u % 2, j] = (gain[:, :1] * part).astype(jnp.bfloat16)
        write(u).start()

    def start_z1(e, m):
        for j in range(blocks):
            @pl.when(g * blocks + j != s)
            def _():
                z1(e, m, j).start()

    def release(u):
        e, m = u // 2, u % 2
        write(u).wait()
        for j in range(blocks):
            x1(e, m, j).start()
        if e == 0:
            start_z1(e, m)

    def round_down(e):
        read_down(e).wait()
        dbounce[...] = dstage[...].astype(jnp.bfloat16)
        for copy in write_down(e):
            copy.start()
        if e + 1 < experts:
            read_down(e + 1).start()
        for copy in write_down(e):
            copy.wait()

    units = 2 * experts
    for u in range(units):
        read(u).start()
    if gain.shape[0] % LANES == 0:
        gain[...] = jnp.broadcast_to(gain_row[...], (8, gain.shape[0])).T
    else:
        gain[...] = jnp.broadcast_to(gain_row[...], gain.shape)
    read_down(0).start()
    barrier = pltpu.get_barrier_semaphore()

    def hello(to):
        pl.semaphore_signal(barrier, inc=1, device_id=to, device_id_type=MESH)

    def greet(k, c):
        at = lax.rem(s + k, n_fs)
        hello(along(at))
        hello(along(at, 1 - tp))
        return c

    lax.fori_loop(1, n_fs, greet, 0)
    hello(partner)
    hello(across)
    hello({"gr": 1 - gr, "fs": s, "tp": 1 - tp})
    pl.semaphore_wait(barrier, 2 * n_fs + 1)

    last = experts - 1
    fetch = pltpu.make_async_copy(tok, nrm, lsem.at[0])
    fetch.start()
    early = min(2, experts)
    with jax.named_scope("cast"):
        for u in range(2 * early):
            round_unit(u)
            if u >= 1:
                release(u - 1)
        release(2 * early - 1)
        round_down(0)
        start_down(0)

    def norm_step(t, carry):
        at = window(t * tile_rows, tile_rows)
        values = nrm[at, :].astype(jnp.float32)
        mean = jnp.mean(values * values, axis=-1, keepdims=True)
        nrm[at, :] = (values * lax.rsqrt(mean + 1e-06)).astype(jnp.bfloat16)
        return carry

    def late():
        with jax.named_scope("late"):
            for u in range(2 * early, units):
                round_unit(u)
                write(u).wait()
            for e in range(1, experts):
                round_down(e)
            sums = weight[:1, :] + weight[1:2, :]
            first, second = weight[:1, :] / sums, weight[1:2, :] / sums
            label = lax.broadcasted_iota(jnp.int32, (8, count), 0)
            mix = jnp.where(route[:1, :] == label, first, 0.0) + jnp.where(route[1:2, :] == label, second, 0.0)
            comb[...] = mix.T
            fetch.wait()
            lax.fori_loop(0, n_fs, norm_step, 0)

    big = 2 * tile_rows

    def more_x(e):
        if e + 2 < experts:
            start_x1(e + 2)

    def more_down(e):
        if e + 1 < experts:
            start_down(e + 1)

    def open_z(e):
        if 0 < e < experts:
            for m in range(2):
                start_z1(e, m)

    def longs(e, start, stop):
        with jax.named_scope(f"long{e}"):
            lax.fori_loop(start, stop, lambda k, c: (long_step(e, k), c)[1], 0)

    def shorts(e):
        with jax.named_scope(f"rdown{e}"):
            relay_down(e)
        with jax.named_scope(f"short{e}"):
            each(lambda k: short_step(e, k))

    half_fs = n_fs // 2
    for e in range(experts):
        @pl.when(receives)
        def _(e=e):
            if e == 0:
                late()
                open_z(1)
                longs(0, 0, half_fs)
                longs(0, half_fs, n_fs)
                more_x(0)
                more_down(0)
                open_z(2)
                if experts > 2:
                    longs(1, 0, half_fs)
            shorts(e)
            if e == 0:
                if experts > 2:
                    longs(1, half_fs, n_fs)
            else:
                more_x(e)
                more_down(e)
                open_z(e + 2)

        @pl.when(off_core != 0)
        def _(e=e):
            if e == 0:
                for ahead in range(experts):
                    with jax.named_scope(f"relay{ahead}"):
                        relay(ahead)
                    if ahead == 0:
                        open_z(1)
                        late()
                    else:
                        if ahead == 1:
                            with jax.named_scope("rdown0"):
                                relay_down(0)
                        open_z(ahead + 1)
                    more_x(ahead)
                    if ahead == 0:
                        more_down(0)
            else:
                more_down(e)
                with jax.named_scope(f"rdown{e}"):
                    relay_down(e)
            with jax.named_scope(f"final{e}"):
                each(lambda k: final_step(e, k))

        with jax.named_scope(f"load{e}"):
            load(e)
        if e < last:
            follow = e + 1 if experts == 2 or e > 0 else experts

            def both(t, carry, e=e, follow=follow):
                tile(e, t * big, big, True)
                if follow < experts:
                    @pl.when(receives)
                    def _():
                        long_step(follow, 2 * t)
                        long_step(follow, 2 * t + 1)

                return carry

            with jax.named_scope(f"dots{e}"):
                lax.fori_loop(0, half_fs, both, 0)

    half = n_hi // 2
    upper = z // half
    step_h = features // 2

    def turn(k):
        crossing = 1 - k // half
        return (upper + crossing * (1 - 2 * upper)) * half + (z + 1 + k) % half

    def to_pair(k, h):
        zt = turn(k)
        return remote(ysend.at[k, h], yrecv.at[zt, h], ys.at[k, h], yr.at[zt, h], along(s + 1 - 2 * y))

    def to_owner(k, h, cross=False):
        zt = (1 - upper) * half + z % half if cross else upper * half + (z + 1 + k) % half
        return remote(zsend.at[k, h], zrecv.at[k, h], zs.at[k, h], zr.at[k, h], along(zt * 2 + y))

    def pair_step(k, carry):
        at = tile(last, (turn(k) * 2 + 1 - y) * tile_rows, tile_rows)
        for h in range(2):
            ysend[k, h] = total[at, h * step_h : (h + 1) * step_h].astype(jnp.bfloat16)
            to_pair(k, h).start()
        return carry

    def summed(at, k, h):
        to_pair(k, h).wait_recv()
        return total[at, h * step_h : (h + 1) * step_h] + yrecv[turn(k), h].astype(jnp.float32)

    def drain_weights():
        for e in range(experts):
            dx(e).wait_send()
            dp(e).wait_send()
            df(e).wait_send()
            for m in range(2):
                for j in range(blocks):
                    x1(e, m, j).wait_send()

                    @pl.when(g * blocks + j != s)
                    def _():
                        z1(e, m, j).wait_send()

                    @pl.when(off_core != 0)
                    def _():
                        for core in range(2):
                            z2(e, m, j, core).wait_send()

                @pl.when(receives)
                def _():
                    def step(k):
                        x2(e, m, k).wait_send()
                        d1(e, m, k).wait_send()
                        d2(e, m, k).wait_send()

                    each(step)

    def halves(h):
        return slice(h * step_h, (h + 1) * step_h)

    def add_arrived(at, h, start, stop):
        def step(k, carry):
            to_owner(k, h).wait_recv()
            total[at, halves(h)] = total[at, halves(h)] + zrecv[k, h].astype(jnp.float32)
            return carry

        lax.fori_loop(start, stop, step, 0)

    def owner_step(k, cross):
        at = tile(last, (turn(k) * 2 + y) * tile_rows, tile_rows)
        for h in range(2):
            if cross:
                total[at, halves(h)] = summed(at, k, h)
                add_arrived(at, h, 0, half - 1)
                zsend[k, h] = total[at, halves(h)].astype(jnp.bfloat16)
            else:
                zsend[k, h] = summed(at, k, h).astype(jnp.bfloat16)
            to_owner(k, h, cross).start()

    def owners(start, stop, cross, lead):
        def step(k, carry):
            if lead:
                pair_step(k + lead, carry)
            owner_step(k, cross)
            return carry

        if stop > start:
            lax.fori_loop(start, stop, step, 0)

    lead = min(2, n_hi - half)
    with jax.named_scope("pairs"):
        lax.fori_loop(0, lead, pair_step, 0)
    with jax.named_scope("owners"):
        owners(0, half - 1, False, lead)
        owners(half - 1, half, True, lead)
        owners(half, n_hi - lead, False, lead)
        owners(n_hi - lead, n_hi - 1, False, 0)
    drain_weights()
    with jax.named_scope("own"):
        at = tile(last, s * tile_rows, tile_rows)
        for h in range(2):
            total[at, halves(h)] = summed(at, n_hi - 1, h)
            add_arrived(at, h, half - 1, n_hi - 1)
    mout[...] = total[at, :].astype(jnp.bfloat16)
    done = pltpu.make_async_copy(mout, mixed_o, lsem.at[0])
    done.start()
    done.wait()

    def drain_pair(k, carry):
        for h in range(2):
            to_pair(k, h).wait_send()
        return carry

    def drain_owner(k, carry):
        for h in range(2):
            to_owner(k, h).wait_send()
        return carry

    lax.fori_loop(0, n_hi, drain_pair, 0)
    lax.fori_loop(0, n_hi - 1, drain_owner, 0)


def make_shards(n_fs, n_group):
    def shards(tokens, gate_master, up_master, down_master, norm_gain, route, route_weight):
        experts, rows, columns = gate_master.shape
        blocks = n_fs // n_group
        width = columns // blocks
        depth = rows * n_fs
        _, count, features = tokens.shape
        high = down_master.shape[2]
        shares = (4, 6) + (2,) * experts
        sides = tuple(16 * max(1, rows * shares[e] // 256) for e in range(experts))
        long = rows - min(sides)
        tile_rows = count // n_fs
        n_hi = n_fs // 2
        units = 2 * experts

        aligned = rows % LANES == 0
        gain = norm_gain[None, :] if aligned else norm_gain[:, None]
        bf16 = jnp.bfloat16
        fused = width % LANES == 0
        parts = width // LANES if fused else 2
        anywhere = pl.BlockSpec(memory_space=pl.ANY)
        dma = pltpu.SemaphoreType.DMA
        gate_out, up_out, down_out, mixed, *_ = pl.pallas_call(
            functools.partial(kernel, n_fs, sides),
            out_shape=(
                jax.ShapeDtypeStruct((experts, depth, width), bf16),
                jax.ShapeDtypeStruct((experts, depth, width), bf16),
                jax.ShapeDtypeStruct((experts, width, n_group * high), bf16),
                jax.ShapeDtypeStruct((tile_rows, features), bf16),
                jax.ShapeDtypeStruct((2, experts, 2, blocks, long, width), bf16),
                jax.ShapeDtypeStruct((experts, blocks, rows, width), bf16),
                jax.ShapeDtypeStruct((experts, blocks, rows, width), bf16),
                jax.ShapeDtypeStruct((experts, width, high), bf16),
            ),
            in_specs=[anywhere] * 4 + [pl.BlockSpec(memory_space=pltpu.VMEM)] * 3,
            out_specs=[anywhere] * 8,
            scratch_shapes=[
                pltpu.VMEM((rows, 8), jnp.float32),
                pltpu.VMEM((count, 8), jnp.float32),
                pltpu.VMEM((count, features), bf16),
                pltpu.VMEM((count, features), jnp.float32),
                pltpu.VMEM((parts, depth, 2 * LANES if fused else width), bf16),
                pltpu.VMEM((width, features), bf16),
                pltpu.VMEM((2 * tile_rows, width), bf16),
                pltpu.VMEM((long, width), bf16),
                pltpu.VMEM((width, high), jnp.float32),
                pltpu.VMEM((width, high), bf16),
                pltpu.VMEM((2, blocks, rows, width), bf16),
                pltpu.VMEM((n_hi, 2, tile_rows, features // 2), bf16),
                pltpu.VMEM((n_hi, 2, tile_rows, features // 2), bf16),
                pltpu.VMEM((n_hi - 1, 2, tile_rows, features // 2), bf16),
                pltpu.VMEM((n_hi - 1, 2, tile_rows, features // 2), bf16),
                pltpu.VMEM((tile_rows, features), bf16),
                dma((units, blocks)), dma((2, units, blocks)), dma((units, blocks)), dma((2, units, blocks)),
                dma((units, n_fs)), dma((units, n_fs)), dma((units, n_fs)), dma((units, n_fs)), dma((units, n_fs)),
                dma((experts,)), dma((experts,)), dma((experts,)), dma((experts,)), dma((experts,)), dma((experts,)),
                dma((n_hi, 2)), dma((n_hi, 2)), dma((n_hi, 2)), dma((n_hi, 2)),
                dma((2 + 2 * parts,)), dma((units,)), dma((2,)), dma((3,)),
            ],
            compiler_params=pltpu.CompilerParams(
                collective_id=0, has_side_effects=True, vmem_limit_bytes=67043328
            ),
        )(tokens[0], gate_master, up_master, down_master, gain, route[0].T, route_weight[0].T)
        return gate_out, up_out, down_out, mixed[None]

    return shards


def solution(mesh):
    n_fs = mesh.shape["fs"]
    n_group = mesh.shape["gr"] * mesh.shape["tp"]
    in_specs = (
        P(GROUP, None, None),
        P(None, "fs", GROUP),
        P(None, "fs", GROUP),
        P(None, "fs", GROUP),
        P("fs"),
        P(GROUP, None, None),
        P(GROUP, None, None),
    )
    out_specs = (
        P(None, None, "fs"),
        P(None, None, "fs"),
        P(None, "fs", None),
        P(GROUP, "fs", None),
    )
    return jax.shard_map(
        make_shards(n_fs, n_group), mesh=mesh, in_specs=in_specs, out_specs=out_specs, check_vma=False
    )
```
